32 devices in a mesh: ep: 16 (over z, y, x), tp: 2 (over core).
Axes of the slice: x: 2, y: 2, z: 4, core: 2. Of those that a mesh axis runs over, the one named last changes fastest.
Arguments:
- tokens: bfloat16 [4096, 4096], P('ep', 'tp'), may hold values from -6 to 6
- norm_gain: float32 [4096], P('tp'), may hold values from 0.5 to 1.5
- expert_gate: bfloat16 [64, 4096, 128], P('ep', 'tp'), may hold values from -0.09375 to 0.09375
- expert_up: bfloat16 [64, 4096, 128], P('ep', 'tp'), may hold values from -0.09375 to 0.09375
- expert_down: bfloat16 [64, 128, 4096], P('ep', None, 'tp'), may hold values from -0.5 to 0.5
- shared_gate: bfloat16 [4096, 128], P('tp'), may hold values from -0.09375 to 0.09375
- shared_up: bfloat16 [4096, 128], P('tp'), may hold values from -0.09375 to 0.09375
- shared_down: bfloat16 [128, 4096], P(None, 'tp'), may hold values from -0.5 to 0.5
- visit_devices: int32 [4096, 4], P('ep'), may hold values from 0 to 15, all different within a row; in each aligned block of 256 rows (0 to 255, 256 to 511, ...) at most 192 rows name the same one
- visit_experts: int32 [4096, 4, 2], P('ep'), may hold values from 0 to 3, all different within a row
- visit_weights: float32 [4096, 4, 2], P('ep'), may hold values from 0.05 to 0.6
Outputs:
- mixed: bfloat16 [4096, 4096], P('ep', 'tp')
The draws below stay inside these ranges and needn't reach their ends.
Inputs may be any that keep to these rules, and one draw needn't show every extreme that they name: `visit_devices`: the 4 groups of one token differ; among the 256 tokens of one index of ep, no group is named by more than 192 tokens, a bound that some block reaches. `visit_experts`: the 2 experts of one visit differ.
All inputs are finite; a program needn't handle non-finite values.
Results may differ from the reference program's by a relative error of at most 0.0015.
Values may be sent and summed in bfloat16 or wider, within the bound.
A program may use at most 128 MiB of HBM per device.

```python
import math
import jax
import jax.numpy as jnp
import numpy as np
from jax import lax

D = 4096
EXP_WIDTH = 128
SHARED_WIDTH = 128
EXP_DEV = 4
GROUP_TOP = 4
PICK = 2
TOK_DEV = 256
TOKENS = 4096
GROUPS = 16
EXPERTS = 64
CAP_DEV = 192


def steps_of(key, dims, pieces, smallest, top_value):
    loudness, own = 1.0, jax.random.fold_in(key, 6)
    for axis_at, parts in pieces:
        steps = jnp.exp(jax.random.uniform(jax.random.fold_in(own, axis_at), (parts,), jnp.float32, smallest / len(pieces), top_value / len(pieces)))
        loudness = loudness * jnp.repeat(steps, dims[axis_at] // parts).reshape([-1 if axis == axis_at else 1 for axis in range(len(dims))])
    return loudness


def choose_distinct(stream_key, rows, amount, top, lift):
    order = jax.random.permutation(jax.random.fold_in(stream_key, 1), amount)
    boost = order
    for power in range(3):
        boost = boost * boost // amount
    boost = boost * lift // amount
    lots = jax.random.randint(jax.random.fold_in(stream_key, 2), (rows, amount), 0, 4096) + boost
    fixed_rows = jax.random.permutation(jax.random.fold_in(stream_key, 3), rows)[jnp.arange(amount) % rows]
    lots = jnp.where(jnp.arange(rows)[:, None] == fixed_rows[None, :], 1 << 14, lots)
    priority = lots * amount + jnp.arange(amount)
    return lax.top_k(priority.astype(jnp.int32), top)[1].astype(jnp.int32)


def routed_block(own_key, own, number, rows, count, top, limit, skew):
    order = jax.random.permutation(own_key, count)
    heavy_load, usual = load_shares(count, rows * top, limit, skew, True), load_shares(count, rows * top, limit, skew, False)
    places = jnp.arange(count)

    def named(tallies, turn):
        used = int((tallies > 0).sum())
        fixed = max(1, used // 4)
        shifted = fixed + (places - fixed + turn * (used - fixed)) % max(1, count - fixed)
        return jnp.zeros((count,), jnp.int32).at[order[jnp.where(places < fixed, places, shifted)]].set(jnp.asarray(tallies, jnp.int32))

    tallies = jnp.where(number % 4 == 0, named(heavy_load, number // 4), named(usual, number - number // 4 - 1))
    mixed = jax.random.permutation(jax.random.fold_in(own, 3), count)
    source_of, receiver = mixed[0:count // 2 * 2:2], mixed[1:count // 2 * 2:2]
    slack = jnp.minimum(tallies[source_of] - 1, limit - tallies[receiver]) // 2
    slack = jnp.where((source_of == order[0]) | (receiver == order[0]) | (tallies[receiver] == 0), 0, jnp.maximum(slack, 0))
    shifted = jax.random.randint(jax.random.fold_in(own, 4), (count // 2,), 0, 1 << 20) % (slack + 1)
    tallies = tallies.at[source_of].add(-shifted).at[receiver].add(shifted)
    labels = jnp.searchsorted(jnp.cumsum(tallies), jnp.arange(rows * top), side="right").astype(jnp.int32)
    grid = labels.reshape(top, rows).T
    grid = grid[jax.random.permutation(jax.random.fold_in(own, 1), rows)]
    turn = jax.random.randint(jax.random.fold_in(own, 2), (rows, 1), 0, top)
    return jnp.take_along_axis(grid, (jnp.arange(top)[None, :] + turn) % top, axis=1)


def load_shares(number_of, total, reach, slope, full):
    portions = [(1 << 20) // math.isqrt(standing ** slope) + 1 for standing in range(1, number_of + 1)]
    largest = reach if full else min(reach, max(-(-total // number_of), total * portions[0] // sum(portions)))
    least = 1 if total - largest >= number_of - 1 else 0
    given, surplus = [largest] + [least] * (number_of - 1), total - largest - least * (number_of - 1)
    while surplus > 0:
        candidates = [i for i in range(1, number_of) if given[i] < largest] or [i for i in range(1, number_of) if given[i] < reach]
        pool, remaining = sum([portions[i] for i in candidates]), surplus
        for i in candidates:
            addition = min(reach - given[i], max(1, remaining * portions[i] // pool), surplus)
            given[i] = given[i] + addition
            surplus = surplus - addition
    return np.array(given)


def centred(own_key, shape, deviation, limit, split=(), kind=jnp.bfloat16):
    result = deviation * jax.random.normal(own_key, shape, jnp.float32)
    if split:
        result = result * steps_of(own_key, shape, split, -0.22, 0.18)
    return jnp.clip(result, -limit, limit).astype(kind)


def setup_inputs(seed: int = 0) -> dict:
    streams_of = jax.random.split(jax.random.key(seed), 12)
    tokens = centred(streams_of[0], (TOKENS, D), 1.0, 6.0, ((0, 16), (1, 2)))
    norm_gain = jnp.clip(1.0 + 0.1 * jax.random.normal(streams_of[1], (D,), jnp.float32), 0.5, 1.5)
    expert_gate = centred(streams_of[2], (EXPERTS, D, EXP_WIDTH), D ** -0.5, 0.09375, ((0, 16), (1, 2)))
    expert_up = centred(streams_of[3], (EXPERTS, D, EXP_WIDTH), D ** -0.5, 0.09375, ((0, 16), (1, 2)))
    expert_down = centred(streams_of[4], (EXPERTS, EXP_WIDTH, D), EXP_WIDTH ** -0.5, 0.5, ((0, 16), (2, 2)))
    shared_gate = centred(streams_of[5], (D, SHARED_WIDTH), D ** -0.5, 0.09375, ((0, 2),))
    shared_up = centred(streams_of[6], (D, SHARED_WIDTH), D ** -0.5, 0.09375, ((0, 2),))
    shared_down = centred(streams_of[7], (SHARED_WIDTH, D), SHARED_WIDTH ** -0.5, 0.5, ((1, 2),))
    visit_devices_keys = jax.random.split(jax.random.fold_in(streams_of[8], 1), TOKENS // TOK_DEV)
    visit_devices_turns = jax.random.permutation(jax.random.fold_in(streams_of[8], 3), TOKENS // TOK_DEV)
    visit_devices = jax.vmap(lambda own, number: routed_block(jax.random.fold_in(streams_of[8], 2), own, number, TOK_DEV, GROUPS, GROUP_TOP, CAP_DEV, 2))(visit_devices_keys, visit_devices_turns).reshape((TOKENS, GROUP_TOP))
    visit_experts = choose_distinct(streams_of[9], TOKENS * GROUP_TOP, EXP_DEV, PICK, 4096).reshape((TOKENS, GROUP_TOP, PICK))
    visit_weights = jnp.clip(jnp.exp(math.log(0.6) - 2.4849067 * jax.random.uniform(streams_of[10], (TOKENS, GROUP_TOP, PICK), jnp.float32) ** steps_of(streams_of[10], (TOKENS, GROUP_TOP, PICK), ((0, 16),), -0.2, 0.2)), 0.05, 0.6)
    return dict(tokens=tokens, norm_gain=norm_gain, expert_gate=expert_gate, expert_up=expert_up, expert_down=expert_down, shared_gate=shared_gate, shared_up=shared_up, shared_down=shared_down, visit_devices=visit_devices, visit_experts=visit_experts, visit_weights=visit_weights)


EPSILON = 1e-06

def swish(value):
    return value / (1.0 + jnp.exp(-value))

def shared_expert(normed, shared_gate, shared_up, shared_down):
    gate_full = jnp.dot(normed, shared_gate, preferred_element_type=jnp.float32)
    upward_full = jnp.dot(normed, shared_up, preferred_element_type=jnp.float32)
    hidden = (swish(gate_full) * upward_full).astype(jnp.bfloat16)
    return jnp.dot(hidden, shared_down, preferred_element_type=jnp.float32)

def reference(tokens, norm_gain, expert_gate, expert_up, expert_down, shared_gate, shared_up, shared_down, visit_devices, visit_experts, visit_weights):
    widened = tokens.astype(jnp.float32)
    inverse = lax.rsqrt(lax.optimization_barrier(jnp.mean(widened * widened, axis=1, keepdims=True)) + EPSILON)
    normed = (widened * inverse * norm_gain[None, :].astype(jnp.float32)).astype(jnp.bfloat16)
    shared_out = shared_expert(normed, shared_gate, shared_up, shared_down)
    count_tokens = tokens.shape[0]
    buffer_rows = GROUPS * CAP_DEV
    chosen = (visit_experts[..., None] == jnp.arange(EXP_DEV, dtype=jnp.int32)).astype(jnp.float32)
    weighting = lax.optimization_barrier(jnp.sum(chosen * visit_weights[..., None].astype(jnp.float32), axis=2))
    weighting = lax.optimization_barrier(weighting.astype(jnp.bfloat16)).astype(jnp.float32)
    padded_rows = jnp.concatenate([normed, jnp.zeros((1, D), jnp.bfloat16)], axis=0)

    def one_group(routed, group):
        matches = visit_devices == group
        gate_here = lax.optimization_barrier(jnp.sum(jnp.where(matches[:, :, None], weighting, jnp.float32(0.0)), axis=1))
        present = jnp.any(matches, axis=1).astype(jnp.int32)
        position = (jnp.cumsum(present) - present).astype(jnp.int32)
        position = jnp.where(present > 0, position, buffer_rows).astype(jnp.int32)
        table = jnp.full((buffer_rows,), count_tokens, jnp.int32).at[position].set(jnp.arange(count_tokens, dtype=jnp.int32), mode='drop')
        gathered = padded_rows[table]
        gate_table = jnp.concatenate([gate_here, jnp.zeros((1, EXP_DEV), jnp.float32)], axis=0)[table]
        first_expert = (group * EXP_DEV).astype(jnp.int32)
        gate_mat = lax.dynamic_slice_in_dim(expert_gate, first_expert, EXP_DEV, 0)
        gate_mat = gate_mat.transpose(1, 0, 2).reshape(D, EXP_DEV * EXP_WIDTH)
        upward_mat = lax.dynamic_slice_in_dim(expert_up, first_expert, EXP_DEV, 0)
        upward_mat = upward_mat.transpose(1, 0, 2).reshape(D, EXP_DEV * EXP_WIDTH)
        down_mat = lax.dynamic_slice_in_dim(expert_down, first_expert, EXP_DEV, 0)
        down_mat = down_mat.reshape(EXP_DEV * EXP_WIDTH, D)
        gate_val = jnp.dot(gathered, gate_mat, preferred_element_type=jnp.float32)
        upward_val = jnp.dot(gathered, upward_mat, preferred_element_type=jnp.float32)
        gate_val = gate_val.reshape(buffer_rows, EXP_DEV, EXP_WIDTH)
        upward_val = upward_val.reshape(buffer_rows, EXP_DEV, EXP_WIDTH)
        activation = (swish(gate_val) * upward_val * gate_table[:, :, None]).astype(jnp.bfloat16)
        produced = jnp.dot(activation.reshape(buffer_rows, EXP_DEV * EXP_WIDTH), down_mat, preferred_element_type=jnp.float32).astype(jnp.bfloat16)
        routed = routed.at[table].add(produced.astype(jnp.float32), mode='drop')
        return (routed, None)
    routed, _ = lax.scan(one_group, jnp.zeros((count_tokens, D), jnp.float32), jnp.arange(GROUPS, dtype=jnp.int32))
    return (routed + shared_out).astype(jnp.bfloat16)
```

```python
import jax
import jax.numpy as jnp
from jax import lax
from jax.sharding import PartitionSpec as P

EPSILON = 1e-06
LOAD = 3
IN_CHUNKS = 4
OUT_CHUNKS = 4


BF16 = jnp.bfloat16
F32 = jnp.float32


def swish(value):
    return value / (1.0 + jnp.exp(-value))


def split_axis(groups):
    line = 1
    while (line * 2) ** 2 <= groups:
        line *= 2
    return line, groups // line


def mm(lhs, rhs):
    return jnp.dot(lhs, rhs, preferred_element_type=F32)


def body(
    tokens,
    norm_gain,
    expert_gate,
    expert_up,
    expert_down,
    shared_gate,
    shared_up,
    shared_down,
    visit_devices,
    visit_experts,
    visit_weights,
):
    count, half = tokens.shape
    groups, cores = lax.axis_size("ep"), lax.axis_size("tp")
    me, core = lax.axis_index("ep"), lax.axis_index("tp")
    visits = visit_devices.shape[1]
    picks = visit_experts.shape[2]
    local, hidden = expert_gate.shape[0], expert_gate.shape[2]
    capacity = LOAD * count * visits // groups
    line, plane = split_axis(groups)
    level, spot = me // plane, me % plane
    swap = [(i, (i + 1) % cores) for i in range(cores)]

    facts = jnp.concatenate(
        [
            visit_devices.T.astype(F32),
            visit_experts.reshape(count, visits * picks).T.astype(F32),
            visit_weights.reshape(count, visits * picks).T,
        ],
        axis=0,
    )
    facts = lax.all_gather(facts, "ep", axis=0, tiled=False)
    homes = facts[:, :visits].astype(jnp.int32)
    experts = facts[:, visits : visits + visits * picks].astype(jnp.int32)
    weights = facts[:, visits + visits * picks :]
    homes_each = jnp.repeat(homes, picks, axis=1)
    gates = jnp.stack(
        [
            jnp.sum(jnp.where((homes_each == me) & (experts == e), weights, 0.0), axis=1)
            for e in range(local)
        ],
        axis=2,
    ).astype(BF16)
    earlier = (jnp.arange(count)[:, None] < jnp.arange(count)[None, :]).astype(BF16)
    slots = jnp.arange(capacity, dtype=jnp.int32)

    def slot_of(mask):
        before = lax.dot_general(
            mask.astype(BF16), earlier, (((mask.ndim - 1,), (0,)), ((), ())),
            preferred_element_type=F32,
        ).astype(jnp.int32)
        return jnp.where(mask, before, -1)

    mine = slot_of(jnp.any(homes == me, axis=1))
    select = (slots[None, :, None] == mine[:, None, :]).astype(BF16)

    widened = tokens.astype(F32)
    squares = lax.psum(jnp.sum(widened * widened, axis=1), "tp")
    inverse = lax.rsqrt(squares / (half * cores) + EPSILON)
    normed = (widened * inverse[:, None] * norm_gain[None, :]).astype(BF16)

    step = half // IN_CHUNKS
    gate_part = up_part = None
    for c in range(IN_CHUNKS):
        cols = slice(c * step, (c + 1) * step)
        every = lax.all_gather(normed[:, cols], "ep", axis=0, tiled=False)
        rows = jnp.einsum("bst,btd->bsd", select, every, preferred_element_type=F32)
        rows = rows.astype(BF16).reshape(groups * capacity, step)
        g = jnp.einsum("rd,edf->ref", rows, expert_gate[:, cols], preferred_element_type=F32)
        u = jnp.einsum("rd,edf->ref", rows, expert_up[:, cols], preferred_element_type=F32)
        gate_part = g if gate_part is None else gate_part + g
        up_part = u if up_part is None else up_part + u

    total = groups * capacity
    keep = total // cores
    gate_rows = jnp.einsum("bst,bte->bse", select, gates, preferred_element_type=F32)
    gate_rows = gate_rows.reshape(total, local)

    def own(array, index):
        return lax.dynamic_slice_in_dim(array, index * keep, keep, 0)

    if cores == 2:
        other = 1 - core
        gate_sum = own(gate_part, core) + lax.ppermute(own(gate_part, other), "tp", swap)
        up_sum = own(up_part, core) + lax.ppermute(own(up_part, other), "tp", swap)
    else:
        gate_sum = lax.psum_scatter(gate_part, "tp", scatter_dimension=0, tiled=True)
        up_sum = lax.psum_scatter(up_part, "tp", scatter_dimension=0, tiled=True)
    act = (swish(gate_sum) * up_sum * own(gate_rows, core)[:, :, None]).astype(BF16)
    act = act.reshape(keep, local * hidden)
    if cores == 2:
        theirs = lax.ppermute(act, "tp", swap)
        first = core == 0
        act = jnp.concatenate(
            [jnp.where(first, act, theirs), jnp.where(first, theirs, act)], axis=0
        )
    else:
        act = lax.all_gather(act, "tp", axis=0, tiled=True)

    s_gate, s_up = lax.psum((mm(normed, shared_gate), mm(normed, shared_up)), "tp")
    s_hidden = (swish(s_gate) * s_up).astype(BF16)

    column = homes.reshape(line, plane, visits, count)
    column = lax.dynamic_index_in_dim(column, spot, 1, keepdims=False)
    merge = []
    for k in range(plane):
        group = level * plane + (spot ^ k)
        place = slot_of(jnp.any(column == group, axis=1))
        merge.append((place[:, :, None] == slots[None, None, :]).astype(BF16))
    merge = jnp.concatenate(merge, axis=2)

    def hop(value, pairs):
        perm = [(a * plane + q, b * plane + q) for a, b in pairs for q in range(plane)]
        return lax.ppermute(value, "ep", perm)

    down = expert_down.reshape(local * hidden, half)
    width = half // OUT_CHUNKS
    outs = []
    for c in range(OUT_CHUNKS):
        cols = slice(c * width, (c + 1) * width)
        made = mm(act, down[:, cols]).astype(BF16).reshape(line, plane, capacity, width)
        got = []
        for k in range(plane):
            piece = lax.dynamic_index_in_dim(made, spot ^ k, 1, keepdims=False)
            if k:
                perm = [(i, i ^ k) for i in range(groups)]
                piece = lax.ppermute(piece, "ep", perm)
            got.append(piece)
        got = jnp.concatenate(got, axis=1)
        sums = jnp.einsum("dts,dsf->dtf", merge, got, preferred_element_type=F32)

        def term(index):
            return lax.dynamic_index_in_dim(
                sums, jnp.clip(index, 0, line - 1), 0, keepdims=False
            )

        up = down_run = None
        for j in range(1, line):
            send_up = term(level + line - j)
            send_down = term(level - line + j)
            if j > 1:
                send_up = send_up + up
                send_down = send_down + down_run
            up = hop(send_up, [(i, i + 1) for i in range(j)])
            down_run = hop(send_down, [(i, i - 1) for i in range(line - j, line)])
        result = term(level) + mm(s_hidden, shared_down[:, cols])
        if up is not None:
            result = result + up + down_run
        outs.append(result.astype(BF16))
    return jnp.concatenate(outs, axis=1)


def solution(mesh):
    placed = (
        P("ep", "tp"),
        P("tp"),
        P("ep", "tp", None),
        P("ep", "tp", None),
        P("ep", None, "tp"),
        P("tp", None),
        P("tp", None),
        P(None, "tp"),
        P("ep", None),
        P("ep", None, None),
        P("ep", None, None),
    )
    return jax.shard_map(body, mesh=mesh, in_specs=placed, out_specs=P("ep", "tp"), check_vma=False)
```
